32 devices in a mesh: ep: 4 (over y, x), tp: 8 (over z, core).
Axes of the slice: x: 2, y: 2, z: 4, core: 2. Of those that a mesh axis runs over, the one named last changes fastest.
Arguments:
- tokens: bfloat16 [768, 4096], P('ep', 'tp'), may hold values from -6 to 6
- cotangent: bfloat16 [768, 4096], P('ep', 'tp'), may hold values from -4 to 4
- routes: int32 [768, 2], P('ep'), may hold values from 0 to 7, all different within a row; in each aligned block of 192 rows (0 to 191, 192 to 383, ...) at most 72 rows name the same one
- gate_weights: bfloat16 [768, 2], P('ep'), may hold values from 0.099609375 to 2.5
- expert_gate: bfloat16 [8, 4096, 1024], P('ep', 'tp'), may hold values from -0.09375 to 0.09375
- expert_up: bfloat16 [8, 4096, 1024], P('ep', 'tp'), may hold values from -0.09375 to 0.09375
- expert_down: bfloat16 [8, 4096, 1024], P('ep', 'tp'), may hold values from -0.1875 to 0.1875
- shared_gate: bfloat16 [4096, 1024], P('tp'), may hold values from -0.09375 to 0.09375
- shared_up: bfloat16 [4096, 1024], P('tp'), may hold values from -0.09375 to 0.09375
- shared_down: bfloat16 [4096, 1024], P('tp'), may hold values from -0.1875 to 0.1875
Outputs:
- token_grad: bfloat16 [768, 4096], P('ep', 'tp')
- gate_grad: bfloat16 [768, 2], P('ep')
- expert_grads: bfloat16 [3, 8, 4096, 1024], P(None, 'ep', 'tp')
- shared_grads: float32 [3, 4096, 1024], P(None, 'tp', 'ep')
- expert_norms: float32 [3, 8, 1024], P(None, 'ep')
- shared_norms: float32 [3, 1024], P(None, 'ep')
The draws below stay inside these ranges and needn't reach their ends.
Inputs may be any that keep to these rules, and one draw needn't show every extreme that they name: `routes`: each row names 2 different experts. In each aligned block of 192 rows no expert is named by more than 72 rows, a bound that some block reaches.
All inputs are finite; a program needn't handle non-finite values.
Results may differ from the reference program's by a relative error of at most 0.0069.
Values may be sent and summed in bfloat16 or wider, within the bound.
A program may use at most 128 MiB of HBM per device.

```python
import math
import jax
import jax.numpy as jnp
import numpy as np
from jax import lax

D = 4096
F = 1024
TOPK = 2
TOK_GRP = 192
EXPERTS = 8
TOKENS = 768
CAP = 72
N_EP = 4
N_TP = 8


def block_levels(rng, extent, cuts, low, high):
    def one(dim, blocks):
        steps = jax.random.uniform(jax.random.fold_in(jax.random.fold_in(rng, 6), dim), (blocks,), jnp.float32, low / len(cuts), high / len(cuts))
        return jnp.repeat(jnp.exp(steps), extent[dim] // blocks).reshape((-1,) + (1,) * (len(extent) - dim - 1))

    gain = one(*cuts[0])
    for cut in cuts[1:]:
        gain = gain * one(*cut)
    return gain


def shared_out(stream_key, own, number, rows, amount, top, limit, lean):
    sequence = jax.random.permutation(stream_key, amount)
    crowded, ordinary = portions_of(amount, rows * top, limit, lean, True), portions_of(amount, rows * top, limit, lean, False)
    places = jnp.arange(amount)

    def named(sizes, turn):
        used = int((sizes > 0).sum())
        fixed = max(1, used // 4)
        passed = fixed + (places - fixed + turn * (used - fixed)) % max(1, amount - fixed)
        return jnp.zeros((amount,), jnp.int32).at[sequence[jnp.where(places < fixed, places, passed)]].set(jnp.asarray(sizes, jnp.int32))

    sizes = jnp.where(number % 4 == 0, named(crowded, number // 4), named(ordinary, number - number // 4 - 1))
    mixed = jax.random.permutation(jax.random.fold_in(own, 3), amount)
    donor, receiver = mixed[0:amount // 2 * 2:2], mixed[1:amount // 2 * 2:2]
    slack = jnp.minimum(sizes[donor] - 1, limit - sizes[receiver]) // 2
    slack = jnp.where((donor == sequence[0]) | (receiver == sequence[0]) | (sizes[receiver] == 0), 0, jnp.maximum(slack, 0))
    passed = jax.random.randint(jax.random.fold_in(own, 4), (amount // 2,), 0, 1 << 20) % (slack + 1)
    sizes = sizes.at[donor].add(-passed).at[receiver].add(passed)
    labels = jnp.searchsorted(jnp.cumsum(sizes), jnp.arange(rows * top), side="right").astype(jnp.int32)
    grid = labels.reshape(top, rows).T
    grid = grid[jax.random.permutation(jax.random.fold_in(own, 1), rows)]
    turn = jax.random.randint(jax.random.fold_in(own, 2), (rows, 1), 0, top)
    return jnp.take_along_axis(grid, (jnp.arange(top)[None, :] + turn) % top, axis=1)


def portions_of(amount, total, most, slope, full):
    portions = [(1 << 20) // math.isqrt(rank ** slope) + 1 for rank in range(1, amount + 1)]
    largest = most if full else min(most, max(-(-total // amount), total * portions[0] // sum(portions)))
    least = 1 if total - largest >= amount - 1 else 0
    counts, spare = [largest] + [least] * (amount - 1), total - largest - least * (amount - 1)
    while spare > 0:
        movable = [i for i in range(1, amount) if counts[i] < largest] or [i for i in range(1, amount) if counts[i] < most]
        whole, budget = sum([portions[i] for i in movable]), spare
        for i in movable:
            extra = min(most - counts[i], max(1, budget * portions[i] // whole), spare)
            counts[i] = counts[i] + extra
            spare = spare - extra
    return np.array(counts)


def noise(own_key, dims, spread, limit, cuts=(), kind=jnp.bfloat16):
    values = spread * jax.random.normal(own_key, dims, jnp.float32)
    if cuts:
        values = values * block_levels(own_key, dims, cuts, -0.22, 0.18)
    return jnp.clip(values, -limit, limit).astype(kind)


def setup_inputs(seed: int = 0) -> dict:
    keys = jax.random.split(jax.random.key(seed), 11)
    tokens = noise(keys[0], (TOKENS, D), 1.0, 6.0, ((0, 4), (1, 8)))
    cotangent = noise(keys[1], (TOKENS, D), 0.5, 4.0, ((0, 4), (1, 8)))
    routes_keys = jax.random.split(jax.random.fold_in(keys[2], 1), TOKENS // TOK_GRP)
    routes_turns = jax.random.permutation(jax.random.fold_in(keys[2], 3), TOKENS // TOK_GRP)
    routes = jax.vmap(lambda own, number: shared_out(jax.random.fold_in(keys[2], 2), own, number, TOK_GRP, EXPERTS, TOPK, CAP, 2))(routes_keys, routes_turns).reshape((TOKENS, TOPK))
    gate_weights = jnp.clip(jnp.exp(math.log(2.5) - 3.2227897 * jax.random.uniform(keys[3], (TOKENS, TOPK), jnp.float32) ** block_levels(keys[3], (TOKENS, TOPK), ((0, 4),), -0.2, 0.2)), 0.099609375, 2.5).astype(jnp.bfloat16)
    expert_gate = noise(keys[4], (EXPERTS, D, F), D ** -0.5, 0.09375, ((0, 4), (1, 8)))
    expert_up = noise(keys[5], (EXPERTS, D, F), D ** -0.5, 0.09375, ((0, 4), (1, 8)))
    expert_down = noise(keys[6], (EXPERTS, D, F), F ** -0.5, 0.1875, ((0, 4), (1, 8)))
    shared_gate = noise(keys[7], (D, F), D ** -0.5, 0.09375, ((0, 8),))
    shared_up = noise(keys[8], (D, F), D ** -0.5, 0.09375, ((0, 8),))
    shared_down = noise(keys[9], (D, F), F ** -0.5, 0.1875, ((0, 8),))
    return dict(tokens=tokens, cotangent=cotangent, routes=routes, gate_weights=gate_weights, expert_gate=expert_gate, expert_up=expert_up, expert_down=expert_down, shared_gate=shared_gate, shared_up=shared_up, shared_down=shared_down)


def block_sum(row_block, weight):
    block_width = row_block.shape[1] // N_TP
    partial_value = jnp.einsum('rbd,bdf->brf', row_block.reshape(row_block.shape[0], N_TP, block_width).astype(jnp.float32), weight.reshape(N_TP, block_width, weight.shape[1]).astype(jnp.float32))
    rounded = lax.optimization_barrier(partial_value.astype(jnp.bfloat16))
    return jnp.sum(rounded.astype(jnp.float32), axis=0)


def row_backward(pre_gate, pre_up, back_act, weights):
    sigmoid_gate = jax.nn.sigmoid(pre_gate)
    silu_gate = pre_gate * sigmoid_gate
    activation = silu_gate * pre_up
    act_grad = weights[:, None] * back_act
    grad_up = (act_grad * silu_gate).astype(jnp.bfloat16)
    grad_gate = (act_grad * pre_up * sigmoid_gate * (1.0 + pre_gate * (1.0 - sigmoid_gate))).astype(jnp.bfloat16)
    scaled_act = (weights[:, None] * activation).astype(jnp.bfloat16)
    weight_grad = jnp.sum(activation * back_act, axis=1).astype(jnp.bfloat16)
    return grad_gate, grad_up, scaled_act, weight_grad


def reference(tokens, cotangent, routes, gate_weights, expert_gate, expert_up, expert_down, shared_gate, shared_up, shared_down):
    per_block = TOK_GRP * TOPK
    flat_expert = routes.reshape(N_EP, per_block)
    onehot = (flat_expert[:, :, None] == jnp.arange(EXPERTS, dtype=jnp.int32)[None, None, :]).astype(jnp.int32)
    position = jnp.sum((jnp.cumsum(onehot, axis=1) - onehot) * onehot, axis=2)
    block_id = jnp.arange(N_EP, dtype=jnp.int32)[:, None]
    global_slot = (flat_expert * (N_EP * CAP) + block_id * CAP + position).reshape(-1).astype(jnp.int32)
    owner_row = (jnp.arange(TOKENS * TOPK, dtype=jnp.int32) // TOPK).astype(jnp.int32)
    slots = EXPERTS * N_EP * CAP
    slot_token = jnp.zeros((slots,), jnp.int32).at[global_slot].set(owner_row)
    slot_live = jnp.zeros((slots,), jnp.bfloat16).at[global_slot].set(jnp.ones((TOKENS * TOPK,), jnp.bfloat16))
    slot_weight = jnp.zeros((slots,), jnp.bfloat16).at[global_slot].set(gate_weights.reshape(-1))

    def expert_pass(packed):
        token_ids, live_rows, row_weights, w_gate, w_up, w_down = packed
        in_tokens = tokens[token_ids] * live_rows[:, None]
        in_cotan = cotangent[token_ids] * live_rows[:, None]
        pre_gate = block_sum(in_tokens, w_gate)
        pre_up = block_sum(in_tokens, w_up)
        back_act = block_sum(in_cotan, w_down)
        grad_gate, grad_up, scaled_act, weight_grad = row_backward(pre_gate, pre_up, back_act, row_weights.astype(jnp.float32))
        slot_grad = (jnp.dot(grad_gate, w_gate.T, preferred_element_type=jnp.float32) + jnp.dot(grad_up, w_up.T, preferred_element_type=jnp.float32)).astype(jnp.bfloat16)
        gate_wgrad = jnp.dot(in_tokens.T, grad_gate, preferred_element_type=jnp.float32)
        up_wgrad = jnp.dot(in_tokens.T, grad_up, preferred_element_type=jnp.float32)
        down_wgrad = jnp.dot(in_cotan.T, scaled_act, preferred_element_type=jnp.float32)
        stacked = jnp.stack([gate_wgrad, up_wgrad, down_wgrad])
        squares = jnp.sum(stacked * stacked, axis=1) / D
        return slot_grad, weight_grad, stacked.astype(jnp.bfloat16), squares

    slot_grads, weight_grads, expert_stack, expert_sq = lax.map(expert_pass, (slot_token.reshape(EXPERTS, N_EP * CAP), slot_live.reshape(EXPERTS, N_EP * CAP), slot_weight.reshape(EXPERTS, N_EP * CAP), expert_gate, expert_up, expert_down))
    routed_rows = slot_grads.reshape(slots, D)[global_slot].astype(jnp.float32)
    routed_sum = jnp.sum(routed_rows.reshape(TOKENS, TOPK, D), axis=1)
    gate_grad = weight_grads.reshape(slots)[global_slot].reshape(TOKENS, TOPK)

    def shared_pass(packed):
        block_tokens, block_cotan = packed
        pre_gate = block_sum(block_tokens, shared_gate)
        pre_up = block_sum(block_tokens, shared_up)
        back_act = block_sum(block_cotan, shared_down)
        grad_gate, grad_up, scaled_act, weight_grad = row_backward(pre_gate, pre_up, back_act, jnp.ones((TOK_GRP,), jnp.float32))
        shared_part = jnp.dot(grad_gate, shared_gate.T, preferred_element_type=jnp.float32) + jnp.dot(grad_up, shared_up.T, preferred_element_type=jnp.float32)
        grads = jnp.stack([jnp.dot(block_tokens.T, grad_gate, preferred_element_type=jnp.float32), jnp.dot(block_tokens.T, grad_up, preferred_element_type=jnp.float32), jnp.dot(block_cotan.T, scaled_act, preferred_element_type=jnp.float32)])
        return shared_part, grads

    shared_parts, shared_blocks = lax.map(shared_pass, (tokens.reshape(N_EP, TOK_GRP, D), cotangent.reshape(N_EP, TOK_GRP, D)))
    token_grad = (routed_sum + shared_parts.reshape(TOKENS, D)).astype(jnp.bfloat16)
    shared_grads = jnp.sum(shared_blocks, axis=0)
    shared_norms = jnp.sum(shared_grads * shared_grads, axis=1) / D
    expert_grads = jnp.transpose(expert_stack, (1, 0, 2, 3))
    expert_norms = jnp.transpose(expert_sq, (1, 0, 2))
    return token_grad, gate_grad, expert_grads, shared_grads, expert_norms, shared_norms
```

```python
import functools

import jax
import jax.numpy as jnp
from jax import lax
from jax.experimental import pallas as pl
from jax.experimental.pallas import tpu as pltpu
from jax.sharding import PartitionSpec as P

MESH = pl.DeviceIdType.MESH
VMEM = pl.BlockSpec(memory_space=pltpu.VMEM)
ROWS = 16
LAG = 2
F32 = jnp.float32
BF16 = jnp.bfloat16


def enter(axis, peers):
    barrier = pltpu.get_barrier_semaphore()
    for peer in peers:
        pl.semaphore_signal(barrier, inc=1, device_id={axis: peer}, device_id_type=MESH)
    return barrier


def gather_kernel(n, tok, cot, meta, tok_out, cot_out, meta_out, send, recv, own):
    me = lax.axis_index("ep")
    peers = [lax.rem(me + s, n) for s in range(1, n)]
    barrier = enter("ep", peers)
    pl.semaphore_wait(barrier, n - 1)
    pairs = ((meta, meta_out), (tok, tok_out), (cot, cot_out))
    copies = []
    for k, (src, dst) in enumerate(pairs):
        for s, peer in enumerate(peers):
            copies.append(
                pltpu.make_async_remote_copy(
                    src_ref=src,
                    dst_ref=dst.at[me],
                    send_sem=send.at[k, s],
                    recv_sem=recv.at[k, s],
                    device_id={"ep": peer},
                    device_id_type=MESH,
                )
            )
    for copy in copies:
        copy.start()
    local = [pltpu.make_async_copy(src, dst.at[me], own.at[k]) for k, (src, dst) in enumerate(pairs)]
    for copy in local:
        copy.start()
    for copy in local:
        copy.wait()
    for copy in copies:
        copy.wait()


def gather_over_ep(tok, cot, meta):
    n = lax.axis_size("ep")
    return pl.pallas_call(
        functools.partial(gather_kernel, n),
        out_shape=[jax.ShapeDtypeStruct((n,) + a.shape, a.dtype) for a in (tok, cot, meta)],
        in_specs=[VMEM] * 3,
        out_specs=[VMEM] * 3,
        scratch_shapes=[
            pltpu.SemaphoreType.DMA((3, n - 1)),
            pltpu.SemaphoreType.DMA((3, n - 1)),
            pltpu.SemaphoreType.DMA((3,)),
        ],
        compiler_params=pltpu.CompilerParams(collective_id=0, has_side_effects=True),
        name="gather_over_ep",
    )(tok, cot, meta)


def line_kernel(n, p, w, g, wg, x, r, t, xs, xr, rs, rr, bs, br, ds, dr, vs, vr, us, ur):
    nz = n // 2
    chunks = p.shape[0] // 4
    hidden = p.shape[2] // 3
    me = lax.axis_index("tp")
    z = me // 2
    c = lax.rem(me, 2)
    partner = z * 2 + 1 - c
    right = lax.rem(z + 1, nz) * 2 + c
    left = lax.rem(z + nz - 1, nz) * 2 + c
    pos = (z, nz - 1 - z)
    onward = (right, left)
    back = (left, right)

    barrier = enter("tp", (partner, right, left))
    pl.semaphore_wait(barrier, 3)

    def remote(src, dst, ss, rsem, peer):
        return pltpu.make_async_remote_copy(
            src_ref=src, dst_ref=dst, send_sem=ss, recv_sem=rsem, device_id={"tp": peer}, device_id_type=MESH
        )

    def swap(d, j):
        return remote(p.at[(d * 2 + 1 - c) * chunks + j], x.at[d * chunks + j], xs.at[d, j], xr.at[d, j], partner)

    def hop(d, j):
        k = d * chunks + j
        return remote(t.at[k], r.at[k], rs.at[d, j], rr.at[d, j], onward[d])

    def own(d, j):
        return (d * 2 + c) * chunks + j

    def spread(d, j):
        k = own(d, j)
        return (
            remote(g.at[k], g.at[k], bs.at[d, j], br.at[d, j], back[d]),
            remote(wg.at[k], wg.at[k], vs.at[d, j], vr.at[d, j], back[d]),
        )

    def share(d, j):
        k = own(d, j)
        return (
            remote(g.at[k], g.at[k], ds.at[d, j], dr.at[d, j], partner),
            remote(wg.at[k], wg.at[k], us.at[d, j], ur.at[d, j], partner),
        )

    def first(j, _):
        for d in range(2):
            swap(d, j).start()
        return 0

    lax.fori_loop(0, chunks, first, 0)

    def step(i, _):
        for d in range(2):
            j = i - LAG * pos[d]
            live = (j >= 0) & (j < chunks)
            k = d * chunks + j
            o = own(d, j)

            @pl.when(live & (pos[d] == 0))
            def _():
                swap(d, j).wait_recv()
                t[k] = (p[o].astype(F32) + x[k].astype(F32)).astype(BF16)

            @pl.when(live & (pos[d] > 0))
            def _():
                swap(d, j).wait_recv()
                hop(d, j).wait_recv()

            @pl.when(live & (pos[d] > 0) & (pos[d] < nz - 1))
            def _():
                t[k] = (p[o].astype(F32) + x[k].astype(F32) + r[k].astype(F32)).astype(BF16)

            @pl.when(live & (pos[d] == nz - 1))
            def _():
                def total(part):
                    cols = pl.ds(part * hidden, hidden)
                    return p[o, :, cols].astype(F32) + x[k, :, cols].astype(F32) + r[k, :, cols].astype(F32)

                gate = total(0)
                up = total(1)
                bk = total(2)
                weight = w[o][:, :1]
                sig = jax.nn.sigmoid(gate)
                silu = gate * sig
                act = silu * up
                act_grad = weight * bk
                g[o, :, 0:hidden] = (act_grad * up * sig * (1.0 + gate * (1.0 - sig))).astype(BF16)
                g[o, :, hidden : 2 * hidden] = (act_grad * silu).astype(BF16)
                g[o, :, 2 * hidden : 3 * hidden] = (weight * act).astype(BF16)
                wg[o] = jnp.broadcast_to(
                    jnp.sum(act * bk, axis=1, keepdims=True), wg.shape[1:]
                ).astype(BF16)

        for d in range(2):
            j = i - LAG * pos[d]
            live = (j >= 0) & (j < chunks)

            @pl.when(live & (pos[d] < nz - 1))
            def _():
                hop(d, j).start()

            @pl.when(live & (pos[d] == nz - 1))
            def _():
                for copy in spread(d, j) + share(d, j):
                    copy.start()

        for d in range(2):
            j = i - LAG * (2 * (nz - 1) - pos[d])
            live = (j >= 0) & (j < chunks) & (pos[d] < nz - 1)

            @pl.when(live)
            def _():
                for copy in spread(d, j):
                    copy.wait_recv()

            @pl.when(live & (pos[d] > 0))
            def _():
                for copy in spread(d, j):
                    copy.start()

            @pl.when(live)
            def _():
                for copy in share(d, j):
                    copy.start()

        return 0

    lax.fori_loop(0, chunks + LAG * 2 * (nz - 1), step, 0)

    def last(j, _):
        for d in range(2):
            swap(d, j).wait_send()
            for copy in share(d, j):
                copy.wait()

            @pl.when(pos[d] < nz - 1)
            def _():
                hop(d, j).wait_send()

            @pl.when(pos[d] > 0)
            def _():
                for copy in spread(d, j):
                    copy.wait_send()

        return 0

    lax.fori_loop(0, chunks, last, 0)


def line_over_tp(p, w):
    n = lax.axis_size("tp")
    chunks = p.shape[0] // 4
    half = (2 * chunks,) + p.shape[1:]
    return pl.pallas_call(
        functools.partial(line_kernel, n),
        out_shape=[
            jax.ShapeDtypeStruct(p.shape, BF16),
            jax.ShapeDtypeStruct(p.shape[:2] + (128,), BF16),
        ],
        in_specs=[VMEM] * 2,
        out_specs=[VMEM] * 2,
        scratch_shapes=[pltpu.VMEM(half, BF16)] * 3 + [pltpu.SemaphoreType.DMA((2, chunks))] * 12,
        compiler_params=pltpu.CompilerParams(
            collective_id=1, has_side_effects=True, vmem_limit_bytes=48 * 2**20
        ),
        name="line_over_tp",
    )(p, w)


def return_kernel(ne, nt, con, gate, sq, tok_out, gate_out, sq_out, rcon, rgate, rsq, cs, cr, gs, gr, qs, qr):
    me = lax.axis_index("ep")
    mt = lax.axis_index("tp")
    ep_peers = [lax.rem(me + s, ne) for s in range(1, ne)]
    tp_peers = [lax.rem(mt + s, nt) for s in range(1, nt)]
    barrier = enter("ep", ep_peers)
    enter("tp", tp_peers)
    pl.semaphore_wait(barrier, ne + nt - 2)

    def remote(src, dst, ss, rsem, axis, peer):
        return pltpu.make_async_remote_copy(
            src_ref=src, dst_ref=dst, send_sem=ss, recv_sem=rsem, device_id={axis: peer}, device_id_type=MESH
        )

    copies = []
    for s, peer in enumerate(ep_peers):
        copies.append(remote(con.at[peer], rcon.at[s], cs.at[s], cr.at[s], "ep", peer))
    for s, peer in enumerate(tp_peers):
        copies.append(remote(sq, rsq.at[s], qs.at[s], qr.at[s], "tp", peer))
    for s, peer in enumerate(ep_peers):
        copies.append(remote(gate.at[peer], rgate.at[s], gs.at[s], gr.at[s], "ep", peer))
    for copy in copies:
        copy.start()
    for copy in copies:
        copy.wait()
    tok_out[...] = (con[me].astype(F32) + sum(rcon[s].astype(F32) for s in range(ne - 1))).astype(BF16)
    gate_out[...] = gate[me] + sum(rgate[s] for s in range(ne - 1))
    sq_out[...] = sq[...] + sum(rsq[s] for s in range(nt - 1))


def return_and_norms(con, gate, sq):
    ne, nt = lax.axis_size("ep"), lax.axis_size("tp")
    return pl.pallas_call(
        functools.partial(return_kernel, ne, nt),
        out_shape=[
            jax.ShapeDtypeStruct(con.shape[1:], BF16),
            jax.ShapeDtypeStruct(gate.shape[1:], F32),
            jax.ShapeDtypeStruct(sq.shape, F32),
        ],
        in_specs=[VMEM] * 3,
        out_specs=[VMEM] * 3,
        scratch_shapes=[
            pltpu.VMEM((ne - 1,) + con.shape[1:], BF16),
            pltpu.VMEM((ne - 1,) + gate.shape[1:], F32),
            pltpu.VMEM((nt - 1,) + sq.shape, F32),
        ]
        + [pltpu.SemaphoreType.DMA((ne - 1,))] * 4
        + [pltpu.SemaphoreType.DMA((nt - 1,))] * 2,
        compiler_params=pltpu.CompilerParams(collective_id=2, has_side_effects=True),
        name="return_and_norms",
    )(con, gate, sq)


def mm(a, b, dims):
    return lax.dot_general(a, b, (dims, ((), ())), preferred_element_type=F32)


def body(
    tokens,
    cotangent,
    routes,
    gate_weights,
    expert_gate,
    expert_up,
    expert_down,
    shared_gate,
    shared_up,
    shared_down,
):
    groups = lax.axis_size("ep")
    lanes = lax.axis_size("tp")
    here, width = tokens.shape
    choose = routes.shape[1]
    local = expert_gate.shape[0]
    hidden = expert_gate.shape[2]
    cap = 3 * here * choose // (2 * local * groups)
    slots = local * groups * cap
    part = hidden // groups
    mine = lax.axis_index("ep")

    meta = jnp.concatenate([routes.T.astype(F32), gate_weights.T.astype(F32)], axis=0)
    tok, cot, meta = gather_over_ep(tokens, cotangent, meta)
    names = meta[:, :choose].astype(jnp.int32)
    gains = meta[:, choose:]
    ids = mine * local + jnp.arange(local, dtype=jnp.int32)
    match = (names[:, None] == ids[None, :, None, None]).astype(F32)
    hit = jnp.sum(match, axis=2)
    gain = jnp.sum(match * gains[:, None], axis=2)
    before = (jnp.arange(here)[:, None] < jnp.arange(here)[None, :]).astype(BF16)
    place = mm(hit.astype(BF16).reshape(groups * local, here), before, ((1,), (0,)))
    place = place.reshape(groups, local, here)
    pick = (
        (place[:, :, None, :] == jnp.arange(cap, dtype=F32)[None, None, :, None]) & (hit[:, :, None, :] > 0)
    ).astype(BF16)
    slot_gain = jnp.sum(pick.astype(F32) * gain[:, :, None, :], axis=3)

    def take(rows, l):
        return jnp.einsum("gct,gtd->gcd", pick[:, l], rows, preferred_element_type=F32).astype(BF16).reshape(
            groups * cap, width
        )

    xs = [take(tok, l) for l in range(local)]
    gs = [take(cot, l) for l in range(local)]

    def columns(weight):
        return lax.dynamic_slice_in_dim(weight, mine * part, part, axis=1)

    sg, su, sd = columns(shared_gate), columns(shared_up), columns(shared_down)

    def side(rows, weight):
        whole = mm(rows.reshape(groups * here, width), weight, ((1,), (0,))).astype(BF16)
        return whole.reshape(groups, here, part).transpose(1, 0, 2).reshape(here, hidden)

    partials = jnp.concatenate(
        [
            jnp.concatenate(
                [
                    mm(xs[l], expert_gate[l], ((1,), (0,))).astype(BF16),
                    mm(xs[l], expert_up[l], ((1,), (0,))).astype(BF16),
                    mm(gs[l], expert_down[l], ((1,), (0,))).astype(BF16),
                ],
                axis=1,
            )
            for l in range(local)
        ]
        + [jnp.concatenate([side(tok, sg), side(tok, su), side(cot, sd)], axis=1)],
        axis=0,
    )
    weights = jnp.concatenate([slot_gain.transpose(1, 0, 2).reshape(slots), jnp.ones((here,), F32)])
    total = slots + here
    weights = jnp.broadcast_to(weights[:, None], (total, 128))
    grads, gate_sum = line_over_tp(
        partials.reshape(total // ROWS, ROWS, 3 * hidden), weights.reshape(total // ROWS, ROWS, 128)
    )
    grads = grads.reshape(total, 3 * hidden)
    gate_sum = gate_sum.reshape(total, 128)[:slots, 0].astype(F32).reshape(local, groups, cap)

    def piece(l, k):
        return grads[l * groups * cap : (l + 1) * groups * cap, k * hidden : (k + 1) * hidden]

    def tall(k):
        block = grads[slots:, k * hidden : (k + 1) * hidden]
        return block.reshape(here, groups, part).transpose(1, 0, 2).reshape(groups * here, part)

    tg, tu, ts = tall(0), tall(1), tall(2)
    con = (mm(tg, sg, ((1,), (1,))) + mm(tu, su, ((1,), (1,)))).reshape(groups, here, width)
    for l in range(local):
        slot_grad = (
            mm(piece(l, 0), expert_gate[l], ((1,), (1,))) + mm(piece(l, 1), expert_up[l], ((1,), (1,)))
        ).astype(BF16)
        con = con + jnp.einsum(
            "gct,gcd->gtd", pick[:, l], slot_grad.reshape(groups, cap, width), preferred_element_type=F32
        )
    con = con.astype(BF16)
    gate_tok = jnp.einsum("glct,lgc->glt", pick.astype(F32), gate_sum, precision=lax.Precision.HIGHEST)
    gate_con = jnp.sum(match * gate_tok[:, :, None], axis=1)

    routed = [
        jnp.stack([mm(xs[l] if k < 2 else gs[l], piece(l, k), ((0,), (0,))) for l in range(local)])
        for k in range(3)
    ]
    flat_tok, flat_cot = tok.reshape(groups * here, width), cot.reshape(groups * here, width)
    shared = [
        mm(flat_tok, tg, ((0,), (0,))),
        mm(flat_tok, tu, ((0,), (0,))),
        mm(flat_cot, ts, ((0,), (0,))),
    ]
    squares = jnp.concatenate(
        [jnp.sum(a * a, axis=1).reshape(-1) for a in routed] + [jnp.sum(a * a, axis=0) for a in shared]
    )
    count = squares.shape[0]
    pad = -count % 1024
    squares = jnp.pad(squares, (0, pad)).reshape(-1, 128)
    token_grad, gate_out, squares = return_and_norms(con, gate_con, squares)
    squares = squares.reshape(-1)[:count] * (1.0 / (width * lanes))
    routed_count = 3 * local * hidden
    return (
        token_grad,
        gate_out.T.astype(BF16),
        jnp.stack(routed).astype(BF16),
        jnp.stack(shared),
        squares[:routed_count].reshape(3, local, hidden),
        squares[routed_count:].reshape(3, part),
    )


def solution(mesh):
    return jax.shard_map(
        body,
        mesh=mesh,
        in_specs=(
            P("ep", "tp"),
            P("ep", "tp"),
            P("ep", None),
            P("ep", None),
            P("ep", "tp", None),
            P("ep", "tp", None),
            P("ep", "tp", None),
            P("tp", None),
            P("tp", None),
            P("tp", None),
        ),
        out_specs=(
            P("ep", "tp"),
            P("ep", None),
            P(None, "ep", "tp", None),
            P(None, "tp", "ep"),
            P(None, "ep", None),
            P(None, "ep"),
        ),
        check_vma=False,
    )
```

```python
import functools

import jax
import jax.numpy as jnp
from jax import lax
from jax.experimental import pallas as pl
from jax.experimental.pallas import tpu as pltpu
from jax.sharding import PartitionSpec as P

MESH = pl.DeviceIdType.MESH
VMEM = pl.BlockSpec(memory_space=pltpu.VMEM)
ROWS = 16
LAG = 2
TILE = 256
F32 = jnp.float32
BF16 = jnp.bfloat16


def enter(axis, peers):
    barrier = pltpu.get_barrier_semaphore()
    for peer in peers:
        pl.semaphore_signal(barrier, inc=1, device_id={axis: peer}, device_id_type=MESH)
    return barrier


def gather_kernel(n, tok, cot, meta, tok_out, cot_out, meta_out, send, recv, own):
    me = lax.axis_index("ep")
    peers = [lax.rem(me + s, n) for s in range(1, n)]
    barrier = enter("ep", peers)
    pl.semaphore_wait(barrier, n - 1)
    pairs = ((meta, meta_out), (tok, tok_out), (cot, cot_out))
    copies = []
    for k, (src, dst) in enumerate(pairs):
        for s, peer in enumerate(peers):
            copies.append(
                pltpu.make_async_remote_copy(
                    src_ref=src,
                    dst_ref=dst.at[me],
                    send_sem=send.at[k, s],
                    recv_sem=recv.at[k, s],
                    device_id={"ep": peer},
                    device_id_type=MESH,
                )
            )
    for copy in copies:
        copy.start()
    local = [pltpu.make_async_copy(src, dst.at[me], own.at[k]) for k, (src, dst) in enumerate(pairs)]
    for copy in local:
        copy.start()
    for copy in local:
        copy.wait()
    for copy in copies:
        copy.wait()


def gather_over_ep(tok, cot, meta):
    n = lax.axis_size("ep")
    return pl.pallas_call(
        functools.partial(gather_kernel, n),
        out_shape=[jax.ShapeDtypeStruct((n,) + a.shape, a.dtype) for a in (tok, cot, meta)],
        in_specs=[VMEM] * 3,
        out_specs=[VMEM] * 3,
        scratch_shapes=[
            pltpu.SemaphoreType.DMA((3, n - 1)),
            pltpu.SemaphoreType.DMA((3, n - 1)),
            pltpu.SemaphoreType.DMA((3,)),
        ],
        compiler_params=pltpu.CompilerParams(collective_id=0, has_side_effects=True),
        name="gather_over_ep",
    )(tok, cot, meta)


def tiles(size):
    step = min(TILE, size)
    return size // step, step


def line_kernel(n, local, *refs):
    rows, refs = (refs[:local], refs[local : 2 * local]), refs[2 * local :]
    tok, cot, eg, eu, ed, sg, su, sd, w, g, p, x, r, t, xs, xr, rs, rr, bs, br, ds, dr = refs
    nz = n // 2
    chunks = p.shape[0] // 4
    hidden = p.shape[2] // 3
    part = sg.shape[1]
    carry = t.dtype
    each = rows[0][0].shape[0] // ROWS
    tail = tok.shape[1] // ROWS
    me = lax.axis_index("tp")
    z = me // 2
    c = lax.rem(me, 2)
    partner = z * 2 + 1 - c
    right = lax.rem(z + 1, nz) * 2 + c
    left = lax.rem(z + nz - 1, nz) * 2 + c
    pos = (z, nz - 1 - z)
    onward = (right, left)
    back = (left, right)

    barrier = enter("tp", (partner, right, left))

    amount, size = tiles(hidden)
    for l in range(local):
        for k, (block, weight) in enumerate(((rows[0][l], eg), (rows[0][l], eu), (rows[1][l], ed))):

            def project(i, _, block=block, weight=weight, k=k, l=l):
                cols = pl.ds(pl.multiple_of(i * size, size), size)
                into = pl.ds(pl.multiple_of(k * hidden + i * size, size), size)
                value = jnp.dot(block[...], weight[l, :, cols], preferred_element_type=F32)
                p[l * each : (l + 1) * each, :, into] = value.astype(BF16).reshape(each, ROWS, size)
                return 0

            lax.fori_loop(0, amount, project, 0)
    for k, (block, weight) in enumerate(((tok, sg), (tok, su), (cot, sd))):
        for b in range(tok.shape[0]):
            value = jnp.dot(block[b], weight[...], preferred_element_type=F32).astype(BF16)
            start = k * hidden + b * part
            p[local * each :, :, start : start + part] = value.reshape(tail, ROWS, part)

    pl.semaphore_wait(barrier, 3)

    def remote(src, dst, ss, rsem, peer):
        return pltpu.make_async_remote_copy(
            src_ref=src, dst_ref=dst, send_sem=ss, recv_sem=rsem, device_id={"tp": peer}, device_id_type=MESH
        )

    def swap(d, j):
        return remote(p.at[(d * 2 + 1 - c) * chunks + j], x.at[d * chunks + j], xs.at[d, j], xr.at[d, j], partner)

    def hop(d, j):
        k = d * chunks + j
        return remote(t.at[k], r.at[k], rs.at[d, j], rr.at[d, j], onward[d])

    def own(d, j):
        return (d * 2 + c) * chunks + j

    def spread(d, j):
        k = own(d, j)
        return (remote(g.at[k], g.at[k], bs.at[d, j], br.at[d, j], back[d]),)

    def share(d, j):
        k = own(d, j)
        return (remote(g.at[k], g.at[k], ds.at[d, j], dr.at[d, j], partner),)

    def first(j, _):
        for d in range(2):
            swap(d, j).start()
        return 0

    lax.fori_loop(0, chunks, first, 0)

    def step(i, _):
        for d in range(2):
            j = i - LAG * pos[d]
            live = (j >= 0) & (j < chunks)
            k = d * chunks + j
            o = own(d, j)

            @pl.when(live & (pos[d] == 0))
            def _():
                swap(d, j).wait_recv()
                t[k] = (p[o].astype(F32) + x[k].astype(F32)).astype(carry)

            @pl.when(live & (pos[d] > 0))
            def _():
                swap(d, j).wait_recv()
                hop(d, j).wait_recv()

            @pl.when(live & (pos[d] > 0) & (pos[d] < nz - 1))
            def _():
                t[k] = (p[o].astype(F32) + x[k].astype(F32) + r[k].astype(F32)).astype(carry)

            @pl.when(live & (pos[d] == nz - 1))
            def _():
                def total(part):
                    cols = pl.ds(part * hidden, hidden)
                    return p[o, :, cols].astype(F32) + x[k, :, cols].astype(F32) + r[k, :, cols].astype(F32)

                gate = total(0)
                up = total(1)
                bk = total(2)
                weight = w[o][:, :1]
                sig = jax.nn.sigmoid(gate)
                silu = gate * sig
                act = silu * up
                act_grad = weight * bk
                g[o, :, 0:hidden] = (act_grad * up * sig * (1.0 + gate * (1.0 - sig))).astype(BF16)
                g[o, :, hidden : 2 * hidden] = (act_grad * silu).astype(BF16)
                g[o, :, 2 * hidden : 3 * hidden] = (weight * act).astype(BF16)
                g[o, :, 3 * hidden :] = jnp.broadcast_to(
                    jnp.sum(act * bk, axis=1, keepdims=True), (ROWS, 128)
                ).astype(BF16)

        for d in range(2):
            j = i - LAG * pos[d]
            live = (j >= 0) & (j < chunks)

            @pl.when(live & (pos[d] < nz - 1))
            def _():
                hop(d, j).start()

            @pl.when(live & (pos[d] == nz - 1))
            def _():
                for copy in spread(d, j) + share(d, j):
                    copy.start()

        for d in range(2):
            j = i - LAG * (2 * (nz - 1) - pos[d])
            live = (j >= 0) & (j < chunks) & (pos[d] < nz - 1)

            @pl.when(live)
            def _():
                for copy in spread(d, j):
                    copy.wait_recv()

            @pl.when(live & (pos[d] > 0))
            def _():
                for copy in spread(d, j):
                    copy.start()

            @pl.when(live)
            def _():
                for copy in share(d, j):
                    copy.start()

        return 0

    lax.fori_loop(0, chunks + LAG * 2 * (nz - 1), step, 0)

    def last(j, _):
        for d in range(2):
            swap(d, j).wait_send()
            for copy in share(d, j):
                copy.wait()

            @pl.when(pos[d] < nz - 1)
            def _():
                hop(d, j).wait_send()

            @pl.when(pos[d] > 0)
            def _():
                for copy in spread(d, j):
                    copy.wait_send()

        return 0

    lax.fori_loop(0, chunks, last, 0)


def line_over_tp(xs, gs, tok, cot, eg, eu, ed, sg, su, sd, w):
    n = lax.axis_size("tp")
    blocks, hidden = w.shape[0], eg.shape[2]
    carry = BF16 if n <= 8 else F32
    full = (blocks, ROWS, 3 * hidden)
    half = (blocks // 2, ROWS, 3 * hidden)
    args = (*xs, *gs, tok, cot, eg, eu, ed, sg, su, sd, w)
    return pl.pallas_call(
        functools.partial(line_kernel, n, len(xs)),
        out_shape=jax.ShapeDtypeStruct((blocks, ROWS, 3 * hidden + 128), BF16),
        in_specs=[VMEM] * len(args),
        out_specs=VMEM,
        scratch_shapes=[
            pltpu.VMEM(full, BF16),
            pltpu.VMEM(half, BF16),
            pltpu.VMEM(half, carry),
            pltpu.VMEM(half, carry),
        ]
        + [pltpu.SemaphoreType.DMA((2, blocks // 4))] * 8,
        compiler_params=pltpu.CompilerParams(
            collective_id=1, has_side_effects=True, vmem_limit_bytes=48 * 2**20
        ),
        name="line_over_tp",
    )(*args)


def return_kernel(ne, nt, local, *refs):
    lhs, refs = (refs[:local], refs[local : 2 * local]), refs[2 * local :]
    tokt, cott, tg, tu, ts, grads, con, gate = refs[:8]
    tok_out, gate_out, sq_out, eg_out, sh_out = refs[8:13]
    sq, rcon, rgate, rsq, cs, cr, gs, gr, qs, qr = refs[13:]
    me = lax.axis_index("ep")
    mt = lax.axis_index("tp")
    ep_peers = [lax.rem(me + s, ne) for s in range(1, ne)]
    tp_peers = [lax.rem(mt + s, nt) for s in range(1, nt)]
    barrier = enter("ep", ep_peers)
    enter("tp", tp_peers)
    pl.semaphore_wait(barrier, ne + nt - 2)

    def remote(src, dst, ss, rsem, axis, peer):
        return pltpu.make_async_remote_copy(
            src_ref=src, dst_ref=dst, send_sem=ss, recv_sem=rsem, device_id={axis: peer}, device_id_type=MESH
        )

    copies = []
    for s, peer in enumerate(ep_peers):
        copies.append(remote(con.at[peer], rcon.at[s], cs.at[s], cr.at[s], "ep", peer))
        copies.append(remote(gate.at[peer], rgate.at[s], gs.at[s], gr.at[s], "ep", peer))
    for copy in copies:
        copy.start()

    sq[...] = jnp.zeros_like(sq)
    hidden = eg_out.shape[3]
    part = sh_out.shape[2]
    each = lhs[0][0].shape[1]
    deep = each // ROWS
    amount, size = tiles(hidden)
    for k, (block, right) in enumerate(((tokt, tg), (tokt, tu), (cott, ts))):
        value = jnp.dot(block[...], right[...], preferred_element_type=F32)
        sh_out[k] = value
        sq[3 * local : 3 * local + 1, k * part : (k + 1) * part] = jnp.sum(value * value, axis=0, keepdims=True)
    for l in range(local):
        for k in range(3):

            def weigh(i, _, k=k, l=l):
                cols = pl.ds(pl.multiple_of(i * size, size), size)
                src = pl.ds(pl.multiple_of(k * hidden + i * size, size), size)
                right = grads[l * deep : (l + 1) * deep, :, src].reshape(each, size)
                value = jnp.dot(lhs[k // 2][l][...], right, preferred_element_type=F32)
                eg_out[k, l, :, cols] = value.astype(BF16)
                sq[k * local + l : k * local + l + 1, cols] = jnp.sum(value * value, axis=0, keepdims=True)
                return 0

            lax.fori_loop(0, amount, weigh, 0)

    sums = [remote(sq, rsq.at[s], qs.at[s], qr.at[s], "tp", peer) for s, peer in enumerate(tp_peers)]
    for copy in sums:
        copy.start()
    for copy in copies:
        copy.wait()
    tok_out[...] = (con[me].astype(F32) + sum(rcon[s].astype(F32) for s in range(ne - 1))).astype(BF16)
    gate_out[...] = gate[me] + sum(rgate[s] for s in range(ne - 1))
    for copy in sums:
        copy.wait()
    sq_out[...] = (sq[...] + sum(rsq[s] for s in range(nt - 1))) * (1.0 / (tokt.shape[0] * nt))


def return_and_norms(xt, gt, tokt, cott, tg, tu, ts, grads, con, gate):
    ne, nt = lax.axis_size("ep"), lax.axis_size("tp")
    local = len(xt)
    width, hidden, part = tokt.shape[0], (grads.shape[2] - 128) // 3, tg.shape[1]
    sq_shape = (-(-(3 * local + 1) // 8) * 8, hidden)
    args = (*xt, *gt, tokt, cott, tg, tu, ts, grads, con, gate)
    return pl.pallas_call(
        functools.partial(return_kernel, ne, nt, local),
        out_shape=[
            jax.ShapeDtypeStruct(con.shape[1:], BF16),
            jax.ShapeDtypeStruct(gate.shape[1:], F32),
            jax.ShapeDtypeStruct(sq_shape, F32),
            jax.ShapeDtypeStruct((3, local, width, hidden), BF16),
            jax.ShapeDtypeStruct((3, width, part), F32),
        ],
        in_specs=[VMEM] * len(args),
        out_specs=[VMEM] * 5,
        scratch_shapes=[
            pltpu.VMEM(sq_shape, F32),
            pltpu.VMEM((ne - 1,) + con.shape[1:], BF16),
            pltpu.VMEM((ne - 1,) + gate.shape[1:], F32),
            pltpu.VMEM((nt - 1,) + sq_shape, F32),
        ]
        + [pltpu.SemaphoreType.DMA((ne - 1,))] * 4
        + [pltpu.SemaphoreType.DMA((nt - 1,))] * 2,
        compiler_params=pltpu.CompilerParams(
            collective_id=2, has_side_effects=True, vmem_limit_bytes=40 * 2**20
        ),
        name="return_and_norms",
    )(*args)


def mm(a, b, dims):
    return lax.dot_general(a, b, (dims, ((), ())), preferred_element_type=F32)


def body(
    tokens,
    cotangent,
    routes,
    gate_weights,
    expert_gate,
    expert_up,
    expert_down,
    shared_gate,
    shared_up,
    shared_down,
):
    groups = lax.axis_size("ep")
    lanes = lax.axis_size("tp")
    here, width = tokens.shape
    choose = routes.shape[1]
    local = expert_gate.shape[0]
    hidden = expert_gate.shape[2]
    cap = 3 * here * choose // (2 * local * groups)
    slots = local * groups * cap
    part = hidden // groups
    mine = lax.axis_index("ep")

    meta = jnp.concatenate([routes.T.astype(F32), gate_weights.T.astype(F32)], axis=0)
    tok, cot, meta = gather_over_ep(tokens, cotangent, meta)
    names = meta[:, :choose].astype(jnp.int32)
    gains = meta[:, choose:]
    ids = mine * local + jnp.arange(local, dtype=jnp.int32)
    match = (names[:, None] == ids[None, :, None, None]).astype(F32)
    hit = jnp.sum(match, axis=2)
    gain = jnp.sum(match * gains[:, None], axis=2)
    before = (jnp.arange(here)[:, None] < jnp.arange(here)[None, :]).astype(BF16)
    place = mm(hit.astype(BF16).reshape(groups * local, here), before, ((1,), (0,)))
    place = place.reshape(groups, local, here)
    pick = (
        (place[:, :, None, :] == jnp.arange(cap, dtype=F32)[None, None, :, None]) & (hit[:, :, None, :] > 0)
    ).astype(BF16)
    slot_gain = jnp.sum(pick.astype(F32) * gain[:, :, None, :], axis=3)

    def take(rows, l):
        return jnp.einsum("gct,gtd->gcd", pick[:, l], rows, preferred_element_type=F32).astype(BF16).reshape(
            groups * cap, width
        )

    xs = [take(tok, l) for l in range(local)]
    gs = [take(cot, l) for l in range(local)]

    def columns(weight):
        return lax.dynamic_slice_in_dim(weight, mine * part, part, axis=1)

    sg, su, sd = columns(shared_gate), columns(shared_up), columns(shared_down)

    weights = jnp.concatenate([slot_gain.transpose(1, 0, 2).reshape(slots), jnp.ones((here,), F32)])
    total = slots + here
    weights = jnp.broadcast_to(weights[:, None], (total, 128))
    blocks = line_over_tp(
        xs,
        gs,
        tok,
        cot,
        expert_gate,
        expert_up,
        expert_down,
        sg,
        su,
        sd,
        weights.reshape(total // ROWS, ROWS, 128),
    )
    grads = blocks.reshape(total, 3 * hidden + 128)
    gate_sum = grads[:slots, 3 * hidden].astype(F32).reshape(local, groups, cap)

    def piece(l, k):
        return grads[l * groups * cap : (l + 1) * groups * cap, k * hidden : (k + 1) * hidden]

    def tall(k):
        block = grads[slots:, k * hidden : (k + 1) * hidden]
        return block.reshape(here, groups, part).transpose(1, 0, 2).reshape(groups * here, part)

    tg, tu, ts = tall(0), tall(1), tall(2)
    con = (mm(tg, sg, ((1,), (1,))) + mm(tu, su, ((1,), (1,)))).reshape(groups, here, width)
    for l in range(local):
        slot_grad = (
            mm(piece(l, 0), expert_gate[l], ((1,), (1,))) + mm(piece(l, 1), expert_up[l], ((1,), (1,)))
        ).astype(BF16)
        con = con + jnp.einsum(
            "gct,gcd->gtd", pick[:, l], slot_grad.reshape(groups, cap, width), preferred_element_type=F32
        )
    con = con.astype(BF16)
    gate_tok = jnp.einsum("glct,lgc->glt", pick.astype(F32), gate_sum, precision=lax.Precision.HIGHEST)
    gate_con = jnp.sum(match * gate_tok[:, :, None], axis=1)

    token_grad, gate_out, squares, routed, shared = return_and_norms(
        [a.T for a in xs],
        [a.T for a in gs],
        tok.reshape(groups * here, width).T,
        cot.reshape(groups * here, width).T,
        tg,
        tu,
        ts,
        blocks,
        con,
        gate_con,
    )
    return (
        token_grad,
        gate_out.T.astype(BF16),
        routed,
        shared,
        squares[: 3 * local].reshape(3, local, hidden),
        squares[3 * local, : 3 * part].reshape(3, part),
    )


def solution(mesh):
    return jax.shard_map(
        body,
        mesh=mesh,
        in_specs=(
            P("ep", "tp"),
            P("ep", "tp"),
            P("ep", None),
            P("ep", None),
            P("ep", "tp", None),
            P("ep", "tp", None),
            P("ep", "tp", None),
            P("tp", None),
            P("tp", None),
            P("tp", None),
        ),
        out_specs=(
            P("ep", "tp"),
            P("ep", None),
            P(None, "ep", "tp", None),
            P(None, "tp", "ep"),
            P(None, "ep", None),
            P(None, "ep"),
        ),
        check_vma=False,
    )
```

```python
import functools

import jax
import jax.numpy as jnp
from jax import lax
from jax.experimental import pallas as pl
from jax.experimental.pallas import tpu as pltpu
from jax.sharding import PartitionSpec as P

MESH = pl.DeviceIdType.MESH
VMEM = pl.BlockSpec(memory_space=pltpu.VMEM)
ROWS = 16
LAG = 2
TILE = 256
F32 = jnp.float32
BF16 = jnp.bfloat16


def enter(axis, peers):
    barrier = pltpu.get_barrier_semaphore()
    for peer in peers:
        pl.semaphore_signal(barrier, inc=1, device_id={axis: peer}, device_id_type=MESH)
    return barrier


def gather_kernel(n, tok, cot, meta, tok_out, cot_out, meta_out, send, recv, own):
    me = lax.axis_index("ep")
    peers = [lax.rem(me + s, n) for s in range(1, n)]
    barrier = enter("ep", peers)
    pl.semaphore_wait(barrier, n - 1)
    pairs = ((meta, meta_out), (tok, tok_out), (cot, cot_out))
    copies = []
    for k, (src, dst) in enumerate(pairs):
        for s, peer in enumerate(peers):
            copies.append(
                pltpu.make_async_remote_copy(
                    src_ref=src,
                    dst_ref=dst.at[me],
                    send_sem=send.at[k, s],
                    recv_sem=recv.at[k, s],
                    device_id={"ep": peer},
                    device_id_type=MESH,
                )
            )
    for copy in copies:
        copy.start()
    local = [pltpu.make_async_copy(src, dst.at[me], own.at[k]) for k, (src, dst) in enumerate(pairs)]
    for copy in local:
        copy.start()
    for copy in local:
        copy.wait()
    for copy in copies:
        copy.wait()


def gather_over_ep(tok, cot, meta):
    n = lax.axis_size("ep")
    return pl.pallas_call(
        functools.partial(gather_kernel, n),
        out_shape=[jax.ShapeDtypeStruct((n,) + a.shape, a.dtype) for a in (tok, cot, meta)],
        in_specs=[VMEM] * 3,
        out_specs=[VMEM] * 3,
        scratch_shapes=[
            pltpu.SemaphoreType.DMA((3, n - 1)),
            pltpu.SemaphoreType.DMA((3, n - 1)),
            pltpu.SemaphoreType.DMA((3,)),
        ],
        compiler_params=pltpu.CompilerParams(collective_id=0, has_side_effects=True),
        name="gather_over_ep",
    )(tok, cot, meta)


def tiles(size):
    step = min(TILE, size)
    return size // step, step


def line_kernel(n, local, *refs):
    rows, refs = (refs[:local], refs[local : 2 * local]), refs[2 * local :]
    tok, cot, eg, eu, ed, sg, su, sd, w, g, p, x, r, t, xs, xr, rs, rr, bs, br, ds, dr = refs
    nz = n // 2
    chunks = p.shape[0] // 4
    hidden = p.shape[2] // 3
    part = sg.shape[1]
    carry = t.dtype
    each = rows[0][0].shape[0] // ROWS
    tail = tok.shape[1] // ROWS
    me = lax.axis_index("tp")
    z = me // 2
    c = lax.rem(me, 2)
    partner = z * 2 + 1 - c
    right = lax.rem(z + 1, nz) * 2 + c
    left = lax.rem(z + nz - 1, nz) * 2 + c
    pos = (z, nz - 1 - z)
    onward = (right, left)
    back = (left, right)

    barrier = enter("tp", (partner, right, left))

    amount, size = tiles(hidden)
    for l in range(local):
        for k, (block, weight) in enumerate(((rows[0][l], eg), (rows[0][l], eu), (rows[1][l], ed))):

            def project(i, _, block=block, weight=weight, k=k, l=l):
                cols = pl.ds(pl.multiple_of(i * size, size), size)
                into = pl.ds(pl.multiple_of(k * hidden + i * size, size), size)
                value = jnp.dot(block[...], weight[l, :, cols], preferred_element_type=F32)
                p[l * each : (l + 1) * each, :, into] = value.astype(BF16).reshape(each, ROWS, size)
                return 0

            lax.fori_loop(0, amount, project, 0)
    for k, (block, weight) in enumerate(((tok, sg), (tok, su), (cot, sd))):
        for b in range(tok.shape[0]):
            value = jnp.dot(block[b], weight[...], preferred_element_type=F32).astype(BF16)
            start = k * hidden + b * part
            p[local * each :, :, start : start + part] = value.reshape(tail, ROWS, part)

    pl.semaphore_wait(barrier, 3)

    def remote(src, dst, ss, rsem, peer):
        return pltpu.make_async_remote_copy(
            src_ref=src, dst_ref=dst, send_sem=ss, recv_sem=rsem, device_id={"tp": peer}, device_id_type=MESH
        )

    def swap(d, j):
        return remote(p.at[(d * 2 + 1 - c) * chunks + j], x.at[d * chunks + j], xs.at[d, j], xr.at[d, j], partner)

    def hop(d, j):
        k = d * chunks + j
        return remote(t.at[k], r.at[k], rs.at[d, j], rr.at[d, j], onward[d])

    def own(d, j):
        return (d * 2 + c) * chunks + j

    def spread(d, j):
        k = own(d, j)
        return (remote(g.at[k], g.at[k], bs.at[d, j], br.at[d, j], back[d]),)

    def share(d, j):
        k = own(d, j)
        return (remote(g.at[k], g.at[k], ds.at[d, j], dr.at[d, j], partner),)

    def first(j, _):
        for d in range(2):
            swap(d, j).start()
        return 0

    lax.fori_loop(0, chunks, first, 0)

    def step(i, _):
        for d in range(2):
            j = i - LAG * pos[d]
            live = (j >= 0) & (j < chunks)
            k = d * chunks + j
            o = own(d, j)

            @pl.when(live & (pos[d] == 0))
            def _():
                swap(d, j).wait_recv()
                t[k] = (p[o].astype(F32) + x[k].astype(F32)).astype(carry)

            @pl.when(live & (pos[d] > 0))
            def _():
                swap(d, j).wait_recv()
                hop(d, j).wait_recv()

            @pl.when(live & (pos[d] > 0) & (pos[d] < nz - 1))
            def _():
                t[k] = (p[o].astype(F32) + x[k].astype(F32) + r[k].astype(F32)).astype(carry)

            @pl.when(live & (pos[d] == nz - 1))
            def _():
                def total(part):
                    cols = pl.ds(part * hidden, hidden)
                    return p[o, :, cols].astype(F32) + x[k, :, cols].astype(F32) + r[k, :, cols].astype(F32)

                gate = total(0)
                up = total(1)
                bk = total(2)
                weight = w[o][:, :1]
                sig = jax.nn.sigmoid(gate)
                silu = gate * sig
                act = silu * up
                act_grad = weight * bk
                g[o, :, 0:hidden] = (act_grad * up * sig * (1.0 + gate * (1.0 - sig))).astype(BF16)
                g[o, :, hidden : 2 * hidden] = (act_grad * silu).astype(BF16)
                g[o, :, 2 * hidden : 3 * hidden] = (weight * act).astype(BF16)
                g[o, :, 3 * hidden :] = jnp.broadcast_to(
                    jnp.sum(act * bk, axis=1, keepdims=True), (ROWS, 128)
                ).astype(BF16)

        for d in range(2):
            j = i - LAG * pos[d]
            live = (j >= 0) & (j < chunks)

            @pl.when(live & (pos[d] < nz - 1))
            def _():
                hop(d, j).start()

            @pl.when(live & (pos[d] == nz - 1))
            def _():
                for copy in spread(d, j) + share(d, j):
                    copy.start()

        for d in range(2):
            j = i - LAG * (2 * (nz - 1) - pos[d])
            live = (j >= 0) & (j < chunks) & (pos[d] < nz - 1)

            @pl.when(live)
            def _():
                for copy in spread(d, j):
                    copy.wait_recv()

            @pl.when(live & (pos[d] > 0))
            def _():
                for copy in spread(d, j):
                    copy.start()

            @pl.when(live)
            def _():
                for copy in share(d, j):
                    copy.start()

        return 0

    lax.fori_loop(0, chunks + LAG * 2 * (nz - 1), step, 0)

    def last(j, _):
        for d in range(2):
            swap(d, j).wait_send()
            for copy in share(d, j):
                copy.wait()

            @pl.when(pos[d] < nz - 1)
            def _():
                hop(d, j).wait_send()

            @pl.when(pos[d] > 0)
            def _():
                for copy in spread(d, j):
                    copy.wait_send()

        return 0

    lax.fori_loop(0, chunks, last, 0)


def line_over_tp(xs, gs, tok, cot, eg, eu, ed, sg, su, sd, w):
    n = lax.axis_size("tp")
    blocks, hidden = w.shape[0], eg.shape[2]
    carry = BF16 if n <= 8 else F32
    full = (blocks, ROWS, 3 * hidden)
    half = (blocks // 2, ROWS, 3 * hidden)
    args = (*xs, *gs, tok, cot, eg, eu, ed, sg, su, sd, w)
    return pl.pallas_call(
        functools.partial(line_kernel, n, len(xs)),
        out_shape=jax.ShapeDtypeStruct((blocks, ROWS, 3 * hidden + 128), BF16),
        in_specs=[VMEM] * len(args),
        out_specs=VMEM,
        scratch_shapes=[
            pltpu.VMEM(full, BF16),
            pltpu.VMEM(half, BF16),
            pltpu.VMEM(half, carry),
            pltpu.VMEM(half, carry),
        ]
        + [pltpu.SemaphoreType.DMA((2, blocks // 4))] * 8,
        compiler_params=pltpu.CompilerParams(
            collective_id=1, has_side_effects=True, vmem_limit_bytes=30 * 2**20
        ),
        name="line_over_tp",
    )(*args)


def return_kernel(ne, nt, local, *refs):
    lhs, refs = (refs[:local], refs[local : 2 * local]), refs[2 * local :]
    tokt, cott, tg, tu, ts, grads, con, gate = refs[:8]
    tok_out, gate_out, sq_out, eg_out, sh_out = refs[8:13]
    sq, rcon, rgate, rsq, cs, cr, gs, gr, qs, qr = refs[13:]
    me = lax.axis_index("ep")
    mt = lax.axis_index("tp")
    ep_peers = [lax.rem(me + s, ne) for s in range(1, ne)]
    tp_peers = [lax.rem(mt + s, nt) for s in range(1, nt)]
    barrier = enter("ep", ep_peers)
    enter("tp", tp_peers)
    pl.semaphore_wait(barrier, ne + nt - 2)

    def remote(src, dst, ss, rsem, axis, peer):
        return pltpu.make_async_remote_copy(
            src_ref=src, dst_ref=dst, send_sem=ss, recv_sem=rsem, device_id={axis: peer}, device_id_type=MESH
        )

    copies = []
    for s, peer in enumerate(ep_peers):
        copies.append(remote(con.at[peer], rcon.at[s], cs.at[s], cr.at[s], "ep", peer))
        copies.append(remote(gate.at[peer], rgate.at[s], gs.at[s], gr.at[s], "ep", peer))
    for copy in copies:
        copy.start()

    sq[...] = jnp.zeros_like(sq)
    hidden = eg_out.shape[3]
    part = sh_out.shape[2]
    each = lhs[0][0].shape[0]
    deep = each // ROWS
    amount, size = tiles(hidden)
    for k, (block, right) in enumerate(((tokt, tg), (tokt, tu), (cott, ts))):
        value = mm(block[...], right[...], ((0,), (0,)))
        sh_out[k] = value
        sq[3 * local : 3 * local + 1, k * part : (k + 1) * part] = jnp.sum(value * value, axis=0, keepdims=True)
    for l in range(local):
        for k in range(3):

            def weigh(i, _, k=k, l=l):
                cols = pl.ds(pl.multiple_of(i * size, size), size)
                src = pl.ds(pl.multiple_of(k * hidden + i * size, size), size)
                right = grads[l * deep : (l + 1) * deep, :, src].reshape(each, size)
                value = mm(lhs[k // 2][l][...], right, ((0,), (0,)))
                eg_out[k, l, :, cols] = value.astype(BF16)
                sq[k * local + l : k * local + l + 1, cols] = jnp.sum(value * value, axis=0, keepdims=True)
                return 0

            lax.fori_loop(0, amount, weigh, 0)

    sums = [remote(sq, rsq.at[s], qs.at[s], qr.at[s], "tp", peer) for s, peer in enumerate(tp_peers)]
    for copy in sums:
        copy.start()
    for copy in copies:
        copy.wait()
    tok_out[...] = (con[me].astype(F32) + sum(rcon[s].astype(F32) for s in range(ne - 1))).astype(BF16)
    gate_out[...] = gate[me] + sum(rgate[s] for s in range(ne - 1))
    for copy in sums:
        copy.wait()
    sq_out[...] = (sq[...] + sum(rsq[s] for s in range(nt - 1))) * (1.0 / (tokt.shape[1] * nt))


def return_and_norms(xt, gt, tokt, cott, tg, tu, ts, grads, con, gate):
    ne, nt = lax.axis_size("ep"), lax.axis_size("tp")
    local = len(xt)
    width, hidden, part = tokt.shape[1], (grads.shape[2] - 128) // 3, tg.shape[1]
    sq_shape = (-(-(3 * local + 1) // 8) * 8, hidden)
    args = (*xt, *gt, tokt, cott, tg, tu, ts, grads, con, gate)
    return pl.pallas_call(
        functools.partial(return_kernel, ne, nt, local),
        out_shape=[
            jax.ShapeDtypeStruct(con.shape[1:], BF16),
            jax.ShapeDtypeStruct(gate.shape[1:], F32),
            jax.ShapeDtypeStruct(sq_shape, F32),
            jax.ShapeDtypeStruct((3, local, width, hidden), BF16),
            jax.ShapeDtypeStruct((3, width, part), F32),
        ],
        in_specs=[VMEM] * len(args),
        out_specs=[VMEM] * 5,
        scratch_shapes=[
            pltpu.VMEM(sq_shape, F32),
            pltpu.VMEM((ne - 1,) + con.shape[1:], BF16),
            pltpu.VMEM((ne - 1,) + gate.shape[1:], F32),
            pltpu.VMEM((nt - 1,) + sq_shape, F32),
        ]
        + [pltpu.SemaphoreType.DMA((ne - 1,))] * 4
        + [pltpu.SemaphoreType.DMA((nt - 1,))] * 2,
        compiler_params=pltpu.CompilerParams(
            collective_id=2, has_side_effects=True, vmem_limit_bytes=24 * 2**20
        ),
        name="return_and_norms",
    )(*args)


def mm(a, b, dims):
    return lax.dot_general(a, b, (dims, ((), ())), preferred_element_type=F32)


def body(
    tokens,
    cotangent,
    routes,
    gate_weights,
    expert_gate,
    expert_up,
    expert_down,
    shared_gate,
    shared_up,
    shared_down,
):
    groups = lax.axis_size("ep")
    lanes = lax.axis_size("tp")
    here, width = tokens.shape
    choose = routes.shape[1]
    local = expert_gate.shape[0]
    hidden = expert_gate.shape[2]
    cap = 3 * here * choose // (2 * local * groups)
    slots = local * groups * cap
    part = hidden // groups
    mine = lax.axis_index("ep")

    meta = jnp.concatenate([routes.T.astype(F32), gate_weights.T.astype(F32)], axis=0)
    tok, cot, meta = gather_over_ep(tokens, cotangent, meta)
    names = meta[:, :choose].astype(jnp.int32)
    gains = meta[:, choose:]
    ids = mine * local + jnp.arange(local, dtype=jnp.int32)
    match = (names[:, None] == ids[None, :, None, None]).astype(F32)
    hit = jnp.sum(match, axis=2)
    gain = jnp.sum(match * gains[:, None], axis=2)
    before = (jnp.arange(here)[:, None] < jnp.arange(here)[None, :]).astype(BF16)
    place = mm(hit.astype(BF16).reshape(groups * local, here), before, ((1,), (0,)))
    place = place.reshape(groups, local, here)
    pick = (
        (place[:, :, None, :] == jnp.arange(cap, dtype=F32)[None, None, :, None]) & (hit[:, :, None, :] > 0)
    ).astype(BF16)
    slot_gain = jnp.sum(pick.astype(F32) * gain[:, :, None, :], axis=3)

    def take(rows, l):
        return jnp.einsum("gct,gtd->gcd", pick[:, l], rows, preferred_element_type=F32).astype(BF16).reshape(
            groups * cap, width
        )

    xs = [take(tok, l) for l in range(local)]
    gs = [take(cot, l) for l in range(local)]

    def columns(weight):
        return lax.dynamic_slice_in_dim(weight, mine * part, part, axis=1)

    sg, su, sd = columns(shared_gate), columns(shared_up), columns(shared_down)

    weights = jnp.concatenate([slot_gain.transpose(1, 0, 2).reshape(slots), jnp.ones((here,), F32)])
    total = slots + here
    weights = jnp.broadcast_to(weights[:, None], (total, 128))
    blocks = line_over_tp(
        xs,
        gs,
        tok,
        cot,
        expert_gate,
        expert_up,
        expert_down,
        sg,
        su,
        sd,
        weights.reshape(total // ROWS, ROWS, 128),
    )
    grads = blocks.reshape(total, 3 * hidden + 128)
    gate_sum = grads[:slots, 3 * hidden].astype(F32).reshape(local, groups, cap)

    def piece(l, k):
        return grads[l * groups * cap : (l + 1) * groups * cap, k * hidden : (k + 1) * hidden]

    def tall(k):
        block = grads[slots:, k * hidden : (k + 1) * hidden]
        return block.reshape(here, groups, part).transpose(1, 0, 2).reshape(groups * here, part)

    tg, tu, ts = tall(0), tall(1), tall(2)
    con = (mm(tg, sg, ((1,), (1,))) + mm(tu, su, ((1,), (1,)))).reshape(groups, here, width)
    for l in range(local):
        slot_grad = (
            mm(piece(l, 0), expert_gate[l], ((1,), (1,))) + mm(piece(l, 1), expert_up[l], ((1,), (1,)))
        ).astype(BF16)
        con = con + jnp.einsum(
            "gct,gcd->gtd", pick[:, l], slot_grad.reshape(groups, cap, width), preferred_element_type=F32
        )
    con = con.astype(BF16)
    gate_tok = jnp.einsum("glct,lgc->glt", pick.astype(F32), gate_sum, precision=lax.Precision.HIGHEST)
    gate_con = jnp.sum(match * gate_tok[:, :, None], axis=1)

    token_grad, gate_out, squares, routed, shared = return_and_norms(
        xs,
        gs,
        tok.reshape(groups * here, width),
        cot.reshape(groups * here, width),
        tg,
        tu,
        ts,
        blocks,
        con,
        gate_con,
    )
    return (
        token_grad,
        gate_out.T.astype(BF16),
        routed,
        shared,
        squares[: 3 * local].reshape(3, local, hidden),
        squares[3 * local, : 3 * part].reshape(3, part),
    )


def solution(mesh):
    return jax.shard_map(
        body,
        mesh=mesh,
        in_specs=(
            P("ep", "tp"),
            P("ep", "tp"),
            P("ep", None),
            P("ep", None),
            P("ep", "tp", None),
            P("ep", "tp", None),
            P("ep", "tp", None),
            P("tp", None),
            P("tp", None),
            P("tp", None),
        ),
        out_specs=(
            P("ep", "tp"),
            P("ep", None),
            P(None, "ep", "tp", None),
            P(None, "tp", "ep"),
            P(None, "ep", None),
            P(None, "ep"),
        ),
        check_vma=False,
    )
```
